32 devices in a mesh: sp: 8 (over z, y), tp: 4 (over x, core).
Axes of the slice: x: 2, y: 2, z: 4, core: 2. Of those that a mesh axis runs over, the one named last changes fastest.
Arguments:
- tokens: bfloat16 [1024, 2048], P(('sp', 'tp')), may hold values from -6 to 6
- norm_gain: float32 [2048], replicated, may hold values from 0.1 to 1.9
- w_query: bfloat16 [2048, 1024], P(None, 'tp'), may hold values from -3 to 3
- w_key: bfloat16 [2048, 1024], P(None, 'tp'), may hold values from -0.15625 to 0.15625
- w_value: bfloat16 [2048, 1024], P(None, 'tp'), may hold values from -0.125 to 0.125
- w_state_in: bfloat16 [2048, 512], P(None, 'tp'), may hold values from -0.125 to 0.125
- decay_rate: float32 [32, 64], P('tp'), may hold values from 0 to 0.04, as said below
- rotation: float32 [32, 64], P('tp'), may hold values from -0.5 to 0.5
- extra_decay: float32 [1024, 32], P('sp', 'tp'), may hold values from -1 to 0, as said below
- in_map: float32 [2, 32, 64, 16], P(None, 'tp'), may hold values from -1 to 1
- out_map: float32 [2, 32, 16, 64], P(None, 'tp'), may hold values from -0.5 to 0.5
- skip_gain: float32 [32, 16], P('tp'), may hold values from -4 to 4
- init_state: float32 [1, 2, 32, 64], P(None, None, 'tp'), may hold values from -6 to 6
- mix_lambda: float32 [8], P('tp'), may hold values from 0.3 to 0.8
- sub_gain: float32 [128], replicated, may hold values from 0.1 to 1.9
- w_out_state: bfloat16 [512, 2048], P('tp', 'sp'), may hold values from -0.375 to 0.375
- w_out_attn: bfloat16 [1024, 2048], P('tp', 'sp'), may hold values from -0.1875 to 0.1875
Outputs:
- mixed_out: bfloat16 [1024, 2048], P(('sp', 'tp'))
The draws below stay inside these ranges and needn't reach their ends.
Inputs may be any that keep to these rules, and one draw needn't show every extreme that they name: `decay_rate`: positive. `extra_decay`: never positive.
All inputs are finite; a program needn't handle non-finite values.
Results may differ from the reference program's by a relative error of at most 0.017.
The reference program's roundings to bfloat16 on the way count: a program that leaves them out, or rounds other values in their place, can miss the bound.
Values may be sent and summed in bfloat16 or wider, within the bound.
A program may use at most 128 MiB of HBM per device.

```python
import math
import jax
import jax.numpy as jnp
from jax import lax

D = 2048
S5_STATE_GROUPS = 32
S5_GROUP = 16
S5_STATE = 64
C_HEADS = 8
QK_DIM = 64
V_DIM = 128
SEGMENT = 64
TOK_DEV = 128
SEQS = 1
S5_WIDTH = 512
C_WIDTH = 1024
TOKEN_TOTAL = 1024
SEQUENCE_LENGTH = 1024
N_TP = 4


def draw_w_query(key, part):
    normal_values = jnp.clip(jax.random.normal(key, (D, 2 * C_HEADS * QK_DIM), jnp.float32), -6.0, 6.0)
    weight_scale = 1.3 / math.sqrt(D)
    return jnp.clip(normal_values * weight_scale, -3.0, 3.0).astype(jnp.bfloat16)


def draw_decay_rate(key, part):
    coin_key, slow_key, fast_key, spread_key = jax.random.split(key, 4)
    slow_share = 0.5
    slow_group = jax.random.uniform(coin_key, (S5_STATE_GROUPS, 1), jnp.float32) < slow_share
    slow_rate = jnp.exp(jax.random.uniform(slow_key, (S5_STATE_GROUPS, 1), jnp.float32, math.log(0.05), math.log(0.3))) / SEQUENCE_LENGTH
    fast_rate = jnp.exp(jax.random.uniform(fast_key, (S5_STATE_GROUPS, 1), jnp.float32, math.log(0.01), math.log(0.03)))
    spread_factor = jnp.exp(jax.random.uniform(spread_key, (S5_STATE_GROUPS, S5_STATE), jnp.float32, -0.2, 0.2))
    return jnp.where(slow_group, slow_rate, fast_rate) * spread_factor


def draw_extra_decay(key, part):
    factor_key, location_key, depth_random_key = jax.random.split(key, 3)
    block_total = TOKEN_TOTAL // TOK_DEV
    block_factor = jnp.exp(jax.random.uniform(factor_key, (block_total, 1, S5_STATE_GROUPS), jnp.float32, math.log(0.5), math.log(2.5)))
    constant_portion = jnp.broadcast_to(block_factor, (block_total, TOK_DEV, S5_STATE_GROUPS)).reshape(TOKEN_TOTAL, S5_STATE_GROUPS) * (-0.3 / SEQUENCE_LENGTH)
    sudden_location = jax.random.uniform(location_key, (TOKEN_TOTAL, S5_STATE_GROUPS), jnp.float32) < 2.0 / SEQUENCE_LENGTH
    sudden_depth = jnp.log(jax.random.uniform(depth_random_key, (TOKEN_TOTAL, S5_STATE_GROUPS), jnp.float32, 0.5, 0.8))
    return jnp.where(sudden_location, sudden_depth, 0.0) + constant_portion


def shard_levels(own_key, dims, cuts, least, high):
    factor_of, own = 1.0, jax.random.fold_in(own_key, 6)
    for axis_at, blocks in cuts:
        heights = jnp.exp(jax.random.uniform(jax.random.fold_in(own, axis_at), (blocks,), jnp.float32, least / len(cuts), high / len(cuts)))
        factor_of = factor_of * jnp.repeat(heights, dims[axis_at] // blocks).reshape([-1 if axis == axis_at else 1 for axis in range(len(dims))])
    return factor_of


def centred(rng, extent, deviation, bound, pieces=(), kind=jnp.bfloat16):
    drawn = deviation * jax.random.normal(rng, extent, jnp.float32)
    if pieces:
        drawn = drawn * shard_levels(rng, extent, pieces, -0.22, 0.18)
    return jnp.clip(drawn, -bound, bound).astype(kind)


def setup_inputs(seed: int = 0) -> dict:
    streams_of = jax.random.split(jax.random.key(seed), 18)
    return {
        "tokens": centred(streams_of[0], (TOKEN_TOTAL, D), 1.0, 6.0, ((0, 32),)),
        "norm_gain": jnp.clip(1.0 + 0.18 * jax.random.normal(streams_of[1], (D,), jnp.float32), 0.1, 1.9),
        "w_query": draw_w_query(jax.random.fold_in(streams_of[17], 71), 0),
        "w_key": centred(streams_of[3], (D, 2 * C_HEADS * QK_DIM), (3 * D // 5) ** -0.5, 0.15625, ((1, 4),)),
        "w_value": centred(streams_of[4], (D, C_WIDTH), D ** -0.5, 0.125, ((1, 4),)),
        "w_state_in": centred(streams_of[5], (D, S5_WIDTH), D ** -0.5, 0.125, ((1, 4),)),
        "decay_rate": draw_decay_rate(jax.random.fold_in(streams_of[17], 71), 0),
        "rotation": jnp.clip(jax.random.uniform(streams_of[7], (S5_STATE_GROUPS, S5_STATE), jnp.float32, -0.5, 0.5) * shard_levels(streams_of[7], (S5_STATE_GROUPS, S5_STATE), ((0, 4),), -0.4, 0.0), -0.5, 0.5),
        "extra_decay": draw_extra_decay(jax.random.fold_in(streams_of[17], 71), 0),
        "in_map": centred(streams_of[9], (2, S5_STATE_GROUPS, S5_STATE, S5_GROUP), (2 * S5_GROUP) ** -0.5, 1.0, ((1, 4),), jnp.float32),
        "out_map": centred(streams_of[10], (2, S5_STATE_GROUPS, S5_GROUP, S5_STATE), (2 * S5_STATE) ** -0.5, 0.5, ((1, 4),), jnp.float32),
        "skip_gain": centred(streams_of[11], (S5_STATE_GROUPS, S5_GROUP), 1.0, 4.0, ((0, 4),), jnp.float32),
        "init_state": centred(streams_of[12], (SEQS, 2, S5_STATE_GROUPS, S5_STATE), 1.5, 6.0, ((2, 4),), jnp.float32),
        "mix_lambda": jnp.clip(0.3 + 0.5 * jax.random.uniform(streams_of[13], (C_HEADS,), jnp.float32) ** shard_levels(streams_of[13], (C_HEADS,), ((0, 4),), -0.2, 0.2), 0.3, 0.8),
        "sub_gain": jnp.clip(1.0 + 0.18 * jax.random.normal(streams_of[14], (V_DIM,), jnp.float32), 0.1, 1.9),
        "w_out_state": centred(streams_of[15], (S5_WIDTH, D), (S5_WIDTH // 2) ** -0.5, 0.375, ((0, 4), (1, 8))),
        "w_out_attn": centred(streams_of[16], (C_WIDTH, D), C_WIDTH ** -0.5, 0.1875, ((0, 4), (1, 8))),
    }


EPSILON = 1e-06
ROTARY_BASE = 10000.0
LAMBDA_INIT = 0.2
MASK_FLOOR = -1e+30

def rotary(values, positions):
    half_width = values.shape[-1] // 2
    inverse = ROTARY_BASE ** (-2.0 * jnp.arange(half_width, dtype=jnp.float32) / values.shape[-1])
    angles = positions.astype(jnp.float32)[:, None] * inverse[None, :]
    cosine_table = jnp.cos(angles)[:, None, :]
    sine_table = jnp.sin(angles)[:, None, :]
    first_half = values[..., :half_width]
    second_half = values[..., half_width:]
    return jnp.concatenate((first_half * cosine_table - second_half * sine_table, first_half * sine_table + second_half * cosine_table), axis=-1)

def chain_combine(earlier, later):
    early_mult_real, early_mult_imag, early_add_real, early_add_imag = earlier
    late_mult_real, late_mult_imag, late_add_real, late_add_imag = later
    return (late_mult_real * early_mult_real - late_mult_imag * early_mult_imag, late_mult_real * early_mult_imag + late_mult_imag * early_mult_real, late_mult_real * early_add_real - late_mult_imag * early_add_imag + late_add_real, late_mult_real * early_add_imag + late_mult_imag * early_add_real + late_add_imag)

def take_sequence(values, sequence):
    blocks = values.reshape((-1, SEQS, TOK_DEV) + values.shape[1:])
    return blocks[:, sequence].reshape((-1,) + values.shape[1:])

def lay_back(parts):
    shaped = [part.reshape((-1, TOK_DEV) + part.shape[1:]) for part in parts]
    stacked = jnp.stack(shaped, axis=1)
    return stacked.reshape((TOKEN_TOTAL,) + parts[0].shape[1:])

def attention(query_heads, key_heads, value_heads, mix_lambda, sub_gain):
    seq_length = query_heads.shape[0]
    block_rows = math.gcd(seq_length, 1024)
    segment_ids = jnp.arange(seq_length, dtype=jnp.int32) // SEGMENT
    outputs = []
    for first_row in range(0, seq_length, block_rows):
        stop_row = first_row + block_rows
        query_block = query_heads[first_row:stop_row].astype(jnp.float32)
        key_block = key_heads[:stop_row].astype(jnp.float32)
        scores = jnp.einsum('qhcd,khcd->hcqk', query_block, key_block) * QK_DIM ** (-0.5)
        allowed = segment_ids[:stop_row][None, :] <= segment_ids[first_row:stop_row][:, None]
        masked = jnp.where(allowed, scores, MASK_FLOOR)
        row_peak = lax.optimization_barrier(jnp.max(masked, axis=-1, keepdims=True))
        exponent = jnp.where(allowed, jnp.exp(masked - row_peak), 0.0)
        totals = lax.optimization_barrier(jnp.sum(exponent, axis=-1))
        rounded = lax.optimization_barrier(exponent.astype(jnp.bfloat16)).astype(jnp.float32)
        numerators = jnp.einsum('hcqk,khd->hcqd', rounded, value_heads[:stop_row].astype(jnp.float32))
        difference = numerators[:, 0] / totals[:, 0, :, None] - mix_lambda[:, None, None] * numerators[:, 1] / totals[:, 1, :, None]
        difference = jnp.transpose(difference, (1, 0, 2))
        normed_heads = difference * lax.rsqrt(lax.optimization_barrier(jnp.mean(difference * difference, axis=-1, keepdims=True)) + EPSILON) * sub_gain * (1.0 - LAMBDA_INIT)
        outputs.append(normed_heads.astype(jnp.bfloat16).reshape(block_rows, -1))
    return jnp.concatenate(outputs, axis=0)

def state_mixer(state_drive, decay_rate, rotation, extra_decay, in_map, out_map, skip_gain, start_state):
    highest = lax.Precision.HIGHEST
    step_count, group_count = extra_decay.shape
    drive_wide = state_drive.astype(jnp.float32).reshape(step_count, group_count, -1)
    magnitude = jnp.exp(extra_decay[:, :, None] - decay_rate[None])
    trans_real = magnitude * jnp.cos(rotation)[None]
    trans_imag = magnitude * jnp.sin(rotation)[None]
    in_scale = jnp.sqrt(-jnp.expm1(-2.0 * decay_rate))
    inject_real = in_scale * jnp.einsum('gnp,tgp->tgn', in_map[0], drive_wide, precision=highest)
    inject_imag = in_scale * jnp.einsum('gnp,tgp->tgn', in_map[1], drive_wide, precision=highest)
    mult_real, mult_imag, add_real, add_imag = lax.associative_scan(chain_combine, (trans_real, trans_imag, inject_real, inject_imag), axis=0)
    state_real = mult_real * start_state[0] - mult_imag * start_state[1] + add_real
    state_imag = mult_real * start_state[1] + mult_imag * start_state[0] + add_imag
    mixed_state = jnp.einsum('gpn,tgn->tgp', out_map[0], state_real, precision=highest) - jnp.einsum('gpn,tgn->tgp', out_map[1], state_imag, precision=highest) + skip_gain * drive_wide
    return jax.nn.gelu(mixed_state).astype(jnp.bfloat16).reshape(step_count, -1)

def reference(tokens, norm_gain, w_query, w_key, w_value, w_state_in, decay_rate, rotation, extra_decay, in_map, out_map, skip_gain, init_state, mix_lambda, sub_gain, w_out_state, w_out_attn):
    tokens_wide = tokens.astype(jnp.float32)
    normed = (tokens_wide * lax.rsqrt(lax.optimization_barrier(jnp.mean(tokens_wide * tokens_wide, axis=-1, keepdims=True)) + EPSILON) * norm_gain).astype(jnp.bfloat16)
    token_ids = jnp.arange(TOKEN_TOTAL, dtype=jnp.int32)
    positions = token_ids // TOK_DEV // SEQS * TOK_DEV + token_ids % TOK_DEV
    query_raw = jnp.dot(normed, w_query, preferred_element_type=jnp.float32).reshape(TOKEN_TOTAL, 2 * C_HEADS, QK_DIM)
    query_heads = rotary(query_raw, positions).astype(jnp.bfloat16).reshape(TOKEN_TOTAL, C_HEADS, 2, QK_DIM)
    key_raw = jnp.dot(normed, w_key, preferred_element_type=jnp.float32).reshape(TOKEN_TOTAL, 2 * C_HEADS, QK_DIM)
    key_heads = rotary(key_raw, positions).astype(jnp.bfloat16).reshape(TOKEN_TOTAL, C_HEADS, 2, QK_DIM)
    value_heads = jnp.dot(normed, w_value, preferred_element_type=jnp.float32).astype(jnp.bfloat16).reshape(TOKEN_TOTAL, C_HEADS, V_DIM)
    state_drive = jnp.dot(normed, w_state_in, preferred_element_type=jnp.float32).astype(jnp.bfloat16)
    attn_parts = []
    state_parts = []
    for sequence in range(SEQS):
        attn_parts.append(attention(take_sequence(query_heads, sequence), take_sequence(key_heads, sequence), take_sequence(value_heads, sequence), mix_lambda, sub_gain))
        state_parts.append(state_mixer(take_sequence(state_drive, sequence), decay_rate, rotation, take_sequence(extra_decay, sequence), in_map, out_map, skip_gain, init_state[sequence]))
    attn_out = lay_back(attn_parts)
    state_out = lay_back(state_parts)
    state_share = S5_WIDTH // N_TP
    attn_share = C_WIDTH // N_TP
    summed = jnp.zeros((TOKEN_TOTAL, D), jnp.float32)
    for head_part in range(N_TP):
        state_cols = state_out[:, head_part * state_share:(head_part + 1) * state_share]
        attn_cols = attn_out[:, head_part * attn_share:(head_part + 1) * attn_share]
        partial_sum = jnp.dot(state_cols, w_out_state[head_part * state_share:(head_part + 1) * state_share], preferred_element_type=jnp.float32) + jnp.dot(attn_cols, w_out_attn[head_part * attn_share:(head_part + 1) * attn_share], preferred_element_type=jnp.float32)
        summed = summed + lax.optimization_barrier(partial_sum.astype(jnp.bfloat16)).astype(jnp.float32)
    return summed.astype(jnp.bfloat16)
```

```python
import functools

import jax
import jax.numpy as jnp
from jax import lax
from jax.experimental import pallas as pl
from jax.experimental.pallas import tpu as pltpu
from jax.sharding import PartitionSpec as P

QK_DIM = 64
V_DIM = 128
SEGMENT = 64
EPSILON = 1e-06
ROTARY_BASE = 10000.0
LAMBDA_INIT = 0.2
MASK_FLOOR = -1e30
F32 = jnp.float32
BF16 = jnp.bfloat16
MESH = pl.DeviceIdType.MESH
HIGHEST = lax.Precision.HIGHEST
EARLY = 3


def dot(a, b, precision=None):
    return jnp.dot(a, b, preferred_element_type=F32, precision=precision)


def dot_t(a, b, precision=None):
    return lax.dot_general(
        a, b, (((1,), (1,)), ((), ())), preferred_element_type=F32, precision=precision
    )


def iota(shape, axis):
    return lax.broadcasted_iota(jnp.int32, shape, axis)


def kernel(
    cfg,
    tokens,
    gain,
    wq_hbm,
    wk_hbm,
    wv_hbm,
    wd_hbm,
    table,
    params,
    extra,
    in_map,
    out_map,
    skip,
    mix,
    sub_gain,
    ws_hbm,
    wa_hbm,
    out,
    xall,
    wq,
    wk,
    wv,
    wd,
    wos,
    woa,
    qz,
    kv,
    summary,
    tr,
    ti,
    ir,
    ii,
    peak,
    total,
    numer,
    part,
    landed,
    acts,
    local_sem,
    x_send,
    x_recv,
    w_send,
    w_recv,
    k_send,
    k_recv,
    s_send,
    s_recv,
    r_send,
    r_recv,
):
    seqs, chain, tps, slots = cfg
    sp = lax.axis_index("sp")
    tp = lax.axis_index("tp")
    li = sp // seqs
    seq = sp % seqs
    own, width = tokens.shape
    rows = own * tps
    heads = wv.shape[1] // V_DIM
    qw = wq.shape[1]
    cols = wos.shape[2]
    flat = tr.shape[1]
    groups = extra.shape[1]
    states = flat // groups
    chans = wd.shape[1]
    per = chans // groups

    pulls = [
        pltpu.make_async_copy(src, dst, local_sem.at[i])
        for i, (src, dst) in enumerate(
            (
                (ws_hbm, wos.at[0]),
                (wa_hbm, woa.at[0]),
                (wd_hbm, wd),
                (wk_hbm, wk),
                (wv_hbm, wv),
                (wq_hbm, wq),
            )
        )
    ]
    for pull in pulls:
        pull.start()

    barrier = pltpu.get_barrier_semaphore()

    def greet_tp(d, _):
        pl.semaphore_signal(
            barrier, inc=1, device_id={"tp": lax.rem(tp + d, tps)}, device_id_type=MESH
        )
        return 0

    def greet_sp(d, _):
        pl.semaphore_signal(
            barrier,
            inc=1,
            device_id={"sp": lax.rem(li + d, chain) * seqs + seq},
            device_id_type=MESH,
        )
        return 0

    lax.fori_loop(1, tps, greet_tp, 0)
    lax.fori_loop(1, chain, greet_sp, 0)

    wide = tokens[...].astype(F32)
    scale = lax.rsqrt(jnp.mean(wide * wide, axis=-1, keepdims=True) + EPSILON)
    xall[tp] = (wide * scale * gain[...]).astype(BF16)

    pl.semaphore_wait(barrier, tps - 1 + chain - 1)

    def x_copy(d):
        return pltpu.make_async_remote_copy(
            src_ref=xall.at[tp],
            dst_ref=xall.at[tp],
            send_sem=x_send.at[d],
            recv_sem=x_recv.at[d],
            device_id={"tp": lax.rem(tp + d, tps)},
            device_id_type=MESH,
        )

    def x_arrival(d):
        source = lax.rem(tp + tps - d, tps)
        return pltpu.make_async_remote_copy(
            src_ref=xall.at[tp],
            dst_ref=xall.at[source],
            send_sem=x_send.at[d],
            recv_sem=x_recv.at[d],
            device_id={"tp": source},
            device_id_type=MESH,
        )

    def w_copies(d):
        peer = {"sp": lax.rem(li + d, chain) * seqs + seq}
        return [
            pltpu.make_async_remote_copy(
                src_ref=ref.at[0],
                dst_ref=ref.at[d],
                send_sem=w_send.at[which, d],
                recv_sem=w_recv.at[which, d],
                device_id=peer,
                device_id_type=MESH,
            )
            for which, ref in enumerate((wos, woa))
        ]

    def chain_copy(ref, send, recv, d):
        return pltpu.make_async_remote_copy(
            src_ref=ref.at[0],
            dst_ref=ref.at[d],
            send_sem=send.at[d],
            recv_sem=recv.at[d],
            device_id={"sp": lax.rem(li + d, chain) * seqs + seq},
            device_id_type=MESH,
        )

    def r_copy(d):
        peer = lax.rem(tp + d, tps)
        return pltpu.make_async_remote_copy(
            src_ref=part.at[peer],
            dst_ref=landed.at[d],
            send_sem=r_send.at[d],
            recv_sem=r_recv.at[d],
            device_id={"tp": peer},
            device_id_type=MESH,
        )

    for d in range(1, tps):
        x_copy(d).start()
    pulls[0].wait()
    pulls[1].wait()

    def push_weights(d, _):
        for copy in w_copies(d):
            copy.start()
        return 0

    early = min(EARLY + 1, slots)
    lax.fori_loop(1, early, push_weights, 0)

    spread = (iota((per, chans), 1) % per == iota((per, chans), 0)).astype(F32)
    in_keep = (iota((flat, chans), 0) // states) == (iota((flat, chans), 1) // per)
    out_keep = (iota((chans, flat), 0) // per) == (iota((chans, flat), 1) // states)
    decay = params[0:1, :]
    lane = iota((rows, 2 * states), 1)
    pieces = [
        jnp.where(lane < states, extra[:, g : g + 1], extra[:, g + 1 : g + 2])
        for g in range(0, groups, 2)
    ]
    magnitude = jnp.exp(jnp.concatenate(pieces, axis=1) - decay)
    tr[...] = magnitude * params[1:2, :]
    ti[...] = magnitude * params[2:3, :]

    for d in range(1, tps):
        x_arrival(d).wait_recv()
    for pull in pulls[2:]:
        pull.wait()
    x = xall[...].reshape(rows, width)

    def turned(raw):
        tiles = []
        half = QK_DIM // 2
        first = (iota((rows, 128), 1) % QK_DIM) < half
        for c in range(0, raw.shape[1], 128):
            v = raw[:, c : c + 128]
            other = jnp.where(first, pltpu.roll(v, 128 - half, 1), pltpu.roll(v, half, 1))
            tiles.append(v * table[:, :128] + other * table[:, 128:])
        return tiles

    for i, tile in enumerate(turned(dot(x, wk[...]))):
        kv[0, :, i * 128 : (i + 1) * 128] = tile.astype(BF16)
    kv[0, :, qw:] = dot(x, wv[...]).astype(BF16)
    drive = dot(x, wd[...]).astype(BF16).astype(F32)

    def push_kv(d, _):
        @pl.when(li + d < chain)
        def _():
            chain_copy(kv, k_send, k_recv, d).start()

        return 0

    lax.fori_loop(1, chain, push_kv, 0)

    for which, ref in enumerate((ir, ii)):
        block = dot(in_map[which * flat : (which + 1) * flat, :], spread, HIGHEST)
        block = jnp.where(in_keep, block, 0.0)
        ref[...] = params[3:4, :] * dot_t(drive, block, HIGHEST)

    def scan_tile(i, carry):
        mr, mi, ar, ai = carry
        at = pl.ds(pl.multiple_of(i * 8, 8), 8)
        a, b, u, v = tr[at, :], ti[at, :], ir[at, :], ii[at, :]
        rows_out = ([], [], [], [])
        for r in range(8):
            p, q = a[r : r + 1], b[r : r + 1]
            mr, mi = p * mr - q * mi, p * mi + q * mr
            ar, ai = (
                p * ar - q * ai + u[r : r + 1],
                p * ai + q * ar + v[r : r + 1],
            )
            for keep, value in zip(rows_out, (mr, mi, ar, ai)):
                keep.append(value)
        for ref, keep in zip((tr, ti, ir, ii), rows_out):
            ref[at, :] = jnp.concatenate(keep, axis=0)
        return mr, mi, ar, ai

    one, zero = jnp.ones((1, flat), F32), jnp.zeros((1, flat), F32)
    mr, mi, ar, ai = lax.fori_loop(0, rows // 8, scan_tile, (one, zero, zero, zero))
    start_r, start_i = params[4:5, :], params[5:6, :]
    head_of_chain = li == 0
    entry_r = mr * start_r - mi * start_i + ar
    entry_i = mr * start_i + mi * start_r + ai
    summary[0] = jnp.concatenate(
        (
            jnp.where(head_of_chain, 0.0, mr),
            jnp.where(head_of_chain, 0.0, mi),
            jnp.where(head_of_chain, entry_r, ar),
            jnp.where(head_of_chain, entry_i, ai),
            zero,
            zero,
            zero,
            zero,
        ),
        axis=0,
    )

    q_tiles = turned(dot(x, wq[...]))
    low = iota((rows, 128), 1) < QK_DIM
    for h in range(heads):
        tile = q_tiles[h].astype(BF16).astype(F32) * QK_DIM**-0.5
        qz[2 * h] = jnp.where(low, tile, 0.0).astype(BF16)
        qz[2 * h + 1] = jnp.where(low, 0.0, tile).astype(BF16)

    def push_summary(d, _):
        @pl.when(li + d < chain)
        def _():
            chain_copy(summary, s_send, s_recv, d).start()

        return 0

    lax.fori_loop(1, chain, push_summary, 0)
    lax.fori_loop(early, slots, push_weights, 0)

    allowed = (iota((rows, rows), 1) // SEGMENT) <= (iota((rows, rows), 0) // SEGMENT)
    for u in range(2 * heads):
        h = u // 2
        s = dot_t(qz[u], kv[0, :, h * 128 : (h + 1) * 128])
        s = jnp.where(allowed, s, MASK_FLOOR)
        m = jnp.max(s, axis=-1, keepdims=True)
        e = jnp.where(allowed, jnp.exp(s - m), 0.0)
        peak[u] = jnp.broadcast_to(m, (rows, V_DIM))
        total[u] = jnp.broadcast_to(jnp.sum(e, axis=-1, keepdims=True), (rows, V_DIM))
        numer[u] = dot(e.astype(BF16), kv[0, :, qw + h * V_DIM : qw + (h + 1) * V_DIM])

    def earlier(j, _):
        @pl.when(j <= li)
        def _():
            chain_copy(kv, k_send, k_recv, j).wait_recv()
            for u in range(2 * heads):
                h = u // 2
                s = dot_t(qz[u], kv[j, :, h * 128 : (h + 1) * 128])
                before = peak[u]
                m = jnp.maximum(before, jnp.max(s, axis=-1, keepdims=True))
                shrink = jnp.exp(before - m)
                e = jnp.exp(s - m[:, :1])
                peak[u] = m
                total[u] = total[u] * shrink + jnp.sum(e, axis=-1, keepdims=True)
                numer[u] = numer[u] * shrink + dot(
                    e.astype(BF16), kv[j, :, qw + h * V_DIM : qw + (h + 1) * V_DIM]
                )

        return 0

    lax.fori_loop(1, chain, earlier, 0)

    for h in range(heads):
        diff = numer[2 * h] / total[2 * h] - mix[h] * (numer[2 * h + 1] / total[2 * h + 1])
        scale = lax.rsqrt(jnp.mean(diff * diff, axis=-1, keepdims=True) + EPSILON)
        acts[:, chans + h * V_DIM : chans + (h + 1) * V_DIM] = (
            diff * scale * sub_gain[...] * (1.0 - LAMBDA_INIT)
        ).astype(BF16)

    def enter(step, carry):
        j = chain - step

        def taken(carry):
            cr, ci = carry
            block = summary[j]
            a, b = block[0:1], block[1:2]
            return a * cr - b * ci + block[2:3], a * ci + b * cr + block[3:4]

        @pl.when(j <= li)
        def _():
            chain_copy(summary, s_send, s_recv, j).wait_recv()

        @pl.when(j > li)
        def _():
            summary[j] = jnp.zeros_like(summary[j])

        return taken(carry)

    cr, ci = lax.fori_loop(1, chain, enter, (zero, zero))
    cr = jnp.where(head_of_chain, start_r, cr)
    ci = jnp.where(head_of_chain, start_i, ci)
    state_r = tr[...] * cr - ti[...] * ci + ir[...]
    state_i = tr[...] * ci + ti[...] * cr + ii[...]
    blocks = [
        jnp.where(
            out_keep,
            jnp.concatenate([out_map[w * chans : (w + 1) * chans, :]] * groups, axis=1),
            0.0,
        )
        for w in range(2)
    ]
    mixed = dot_t(state_r, blocks[0], HIGHEST) - dot_t(state_i, blocks[1], HIGHEST)
    acts[:, :chans] = jax.nn.gelu(mixed + skip[...] * drive).astype(BF16)

    def project(j, _):
        if slots > 1:

            @pl.when(j > 0)
            def _():
                for copy in w_copies(j):
                    copy.wait_recv()

        block = dot(acts[:, :chans], wos[j]) + dot(acts[:, chans:], woa[j])
        at = pl.multiple_of(lax.rem(sp + slots - j, slots) * cols, 128)
        part[:, :, pl.ds(at, cols)] = block.astype(BF16).reshape(tps, own, cols)
        return 0

    lax.fori_loop(0, slots, project, 0)
    for d in range(1, tps):
        r_copy(d).start()
    summed = part[tp].astype(F32)
    for d in range(1, tps):
        r_copy(d).wait_recv()
        summed = summed + landed[d].astype(F32)
    out[...] = summed.astype(BF16)

    for d in range(1, tps):
        x_copy(d).wait_send()
        r_copy(d).wait_send()

    def drain(d, _):
        @pl.when(li + d < chain)
        def _():
            chain_copy(kv, k_send, k_recv, d).wait_send()
            chain_copy(summary, s_send, s_recv, d).wait_send()

        return 0

    lax.fori_loop(1, chain, drain, 0)

    def drain_weights(d, _):
        for copy in w_copies(d):
            copy.wait_send()
        return 0

    lax.fori_loop(1, slots, drain_weights, 0)


def local(
    mesh_shape,
    tokens,
    norm_gain,
    w_query,
    w_key,
    w_value,
    w_state_in,
    decay_rate,
    rotation,
    extra_decay,
    in_map,
    out_map,
    skip_gain,
    init_state,
    mix_lambda,
    sub_gain,
    w_out_state,
    w_out_attn,
):
    sps, tps = mesh_shape
    seqs = init_state.shape[0]
    chain = sps // seqs
    own, width = tokens.shape
    rows = own * tps
    if rows % SEGMENT:
        raise ValueError("rows")
    groups, states = decay_rate.shape
    flat = groups * states
    chans = w_state_in.shape[1]
    qw = w_query.shape[1]
    vw = w_value.shape[1]
    units = 2 * vw // V_DIM
    sp = lax.axis_index("sp")
    if seqs == 1 and w_out_state.shape[1] % 128 == 0:
        slots = sps
    else:
        slots = 1
        w_out_state = lax.all_gather(w_out_state, "sp", axis=1, tiled=True)
        w_out_attn = lax.all_gather(w_out_attn, "sp", axis=1, tiled=True)
    cols = w_out_state.shape[1]

    half = QK_DIM // 2
    inverse = ROTARY_BASE ** (-2.0 * jnp.arange(half, dtype=F32) / QK_DIM)
    positions = ((sp // seqs) * rows + jnp.arange(rows, dtype=jnp.int32)).astype(F32)
    angles = positions[:, None] * inverse[None, :]
    cosine, sine = jnp.cos(angles), jnp.sin(angles)
    copies = 128 // QK_DIM
    table = jnp.concatenate((cosine, cosine) * copies + (-sine, sine) * copies, axis=1)

    start = lax.dynamic_index_in_dim(init_state, sp % seqs, 0, keepdims=False)
    zero = jnp.zeros((1, flat), F32)
    params = jnp.concatenate(
        (
            decay_rate.reshape(1, flat),
            jnp.cos(rotation).reshape(1, flat),
            jnp.sin(rotation).reshape(1, flat),
            jnp.sqrt(-jnp.expm1(-2.0 * decay_rate)).reshape(1, flat),
            start.reshape(2, flat),
            zero,
            zero,
        ),
        axis=0,
    )

    vmem = pl.BlockSpec(memory_space=pltpu.VMEM)
    hbm = pl.BlockSpec(memory_space=pl.ANY)
    smem = pl.BlockSpec(memory_space=pltpu.SMEM)
    dma = pltpu.SemaphoreType.DMA
    return pl.pallas_call(
        functools.partial(kernel, (seqs, chain, tps, slots)),
        out_shape=jax.ShapeDtypeStruct((own, width), BF16),
        in_specs=[vmem, vmem, hbm, hbm, hbm, hbm]
        + [vmem] * 6
        + [smem, vmem, hbm, hbm],
        out_specs=vmem,
        scratch_shapes=[
            pltpu.VMEM((tps, own, width), BF16),
            pltpu.VMEM(w_query.shape, BF16),
            pltpu.VMEM(w_key.shape, BF16),
            pltpu.VMEM(w_value.shape, BF16),
            pltpu.VMEM(w_state_in.shape, BF16),
            pltpu.VMEM((slots,) + w_out_state.shape, BF16),
            pltpu.VMEM((slots,) + w_out_attn.shape, BF16),
            pltpu.VMEM((units, rows, 128), BF16),
            pltpu.VMEM((chain, rows, qw + vw), BF16),
            pltpu.VMEM((chain, 8, flat), F32),
            pltpu.VMEM((rows, flat), F32),
            pltpu.VMEM((rows, flat), F32),
            pltpu.VMEM((rows, flat), F32),
            pltpu.VMEM((rows, flat), F32),
            pltpu.VMEM((units, rows, V_DIM), F32),
            pltpu.VMEM((units, rows, V_DIM), F32),
            pltpu.VMEM((units, rows, V_DIM), F32),
            pltpu.VMEM((tps, own, width), BF16),
            pltpu.VMEM((tps, own, width), BF16),
            pltpu.VMEM((rows, chans + vw), BF16),
            dma((6,)),
            dma((tps,)),
            dma((tps,)),
            dma((2, slots)),
            dma((2, slots)),
            dma((chain,)),
            dma((chain,)),
            dma((chain,)),
            dma((chain,)),
            dma((tps,)),
            dma((tps,)),
        ],
        compiler_params=pltpu.CompilerParams(
            collective_id=0, has_side_effects=True, vmem_limit_bytes=48 * 1024 * 1024
        ),
    )(
        tokens,
        norm_gain.reshape(1, width),
        w_query,
        w_key,
        w_value,
        w_state_in,
        table,
        params,
        extra_decay,
        in_map.reshape(2 * flat, chans // groups),
        out_map.reshape(2 * chans, states),
        skip_gain.reshape(1, chans),
        mix_lambda,
        sub_gain.reshape(1, V_DIM),
        w_out_state,
        w_out_attn,
    )


def solution(mesh):
    in_specs = (
        P(("sp", "tp"), None),
        P(),
        P(None, "tp"),
        P(None, "tp"),
        P(None, "tp"),
        P(None, "tp"),
        P("tp", None),
        P("tp", None),
        P("sp", "tp"),
        P(None, "tp", None, None),
        P(None, "tp", None, None),
        P("tp", None),
        P(None, None, "tp", None),
        P("tp"),
        P(),
        P("tp", "sp"),
        P("tp", "sp"),
    )
    shape = (mesh.shape["sp"], mesh.shape["tp"])
    return jax.shard_map(
        functools.partial(local, shape),
        mesh=mesh,
        in_specs=in_specs,
        out_specs=P(("sp", "tp"), None),
        check_vma=False,
    )
```

```python
import functools
import math

import jax
import jax.numpy as jnp
from jax import lax
from jax.experimental import pallas as pl
from jax.experimental.pallas import tpu as pltpu
from jax.sharding import PartitionSpec as P

QK_DIM = 64
V_DIM = 128
SEGMENT = 64
EPSILON = 1e-06
ROTARY_BASE = 10000.0
LAMBDA_INIT = 0.2
MASK_FLOOR = -1e30
F32 = jnp.float32
BF16 = jnp.bfloat16
MESH = pl.DeviceIdType.MESH
HIGHEST = lax.Precision.HIGHEST


def dot(a, b, precision=None):
    return jnp.dot(a, b, preferred_element_type=F32, precision=precision)


def dot_t(a, b, precision=None):
    return lax.dot_general(
        a, b, (((1,), (1,)), ((), ())), preferred_element_type=F32, precision=precision
    )


def one_less_exp(x):
    series = jnp.ones_like(x)
    for n in range(9, 1, -1):
        series = 1.0 - x * series * (1.0 / n)
    return jnp.where(x < 0.5, x * series, 1.0 - jnp.exp(-x))


def iota(shape, axis):
    return lax.broadcasted_iota(jnp.int32, shape, axis)


def kernel(
    cfg,
    tokens,
    gain,
    wq_hbm,
    wk_hbm,
    wv_hbm,
    wd_hbm,
    decay_in,
    turn_in,
    start_in,
    extra_t,
    in_map,
    out_map,
    skip,
    mix,
    sub_gain,
    ws_hbm,
    wa_hbm,
    out,
    xall,
    wq,
    wk,
    wv,
    wd,
    wo,
    qz,
    kv,
    summary,
    tr,
    ti,
    ir,
    ii,
    peak,
    total,
    numer,
    part,
    landed,
    acts,
    local_sem,
    x_send,
    x_recv,
    wu_send,
    wd_send,
    wy_send,
    wz_recv,
    wy_recv,
    ku_send,
    ky_send,
    kz_recv,
    ky_recv,
    s_send,
    s_recv,
    r_send,
    r_recv,
):
    seqs, chain, tps, fold, gather = cfg
    reach = chain // fold
    sp = lax.axis_index("sp")
    tp = lax.axis_index("tp")
    li = sp // seqs
    seq = sp % seqs
    zi, yi = li // fold, li % fold
    own, width = tokens.shape
    rows = own * tps
    heads = wv.shape[1] // V_DIM
    qw = wq.shape[1]
    cols = wo.shape[3]
    flat = tr.shape[1]
    groups = extra_t.shape[0]
    states = flat // groups
    chans = wd.shape[1]
    per = chans // groups

    pulls = [
        pltpu.make_async_copy(src, dst, local_sem.at[i])
        for i, (src, dst) in enumerate(
            (
                (ws_hbm, wo.at[0, 0, pl.ds(0, chans)]),
                (wa_hbm, wo.at[0, 0, pl.ds(chans, wa_hbm.shape[0])]),
                (wd_hbm, wd),
                (wk_hbm, wk),
                (wv_hbm, wv),
                (wq_hbm, wq),
            )
        )
    ]
    for pull in pulls:
        pull.start()

    barrier = pltpu.get_barrier_semaphore()

    def greet_tp(d, _):
        pl.semaphore_signal(
            barrier, inc=1, device_id={"tp": lax.rem(tp + d, tps)}, device_id_type=MESH
        )
        return 0

    def greet_sp(d, _):
        pl.semaphore_signal(
            barrier,
            inc=1,
            device_id={"sp": lax.rem(li + d, chain) * seqs + seq},
            device_id_type=MESH,
        )
        return 0

    lax.fori_loop(1, tps, greet_tp, 0)
    lax.fori_loop(1, chain, greet_sp, 0)

    wide = tokens[...].astype(F32)
    scale = lax.rsqrt(jnp.mean(wide * wide, axis=-1, keepdims=True) + EPSILON)
    xall[tp] = (wide * scale * gain[...]).astype(BF16)

    pl.semaphore_wait(barrier, tps - 1 + chain - 1)

    def send(src, dst, send_sem, recv_sem, device_id):
        return pltpu.make_async_remote_copy(
            src_ref=src,
            dst_ref=dst,
            send_sem=send_sem,
            recv_sem=recv_sem,
            device_id=device_id,
            device_id_type=MESH,
        )

    def at_chain(z, y):
        return {"sp": (z * fold + y) * seqs + seq}

    above = at_chain(lax.rem(zi + 1, reach), yi)
    below = at_chain(lax.rem(zi + reach - 1, reach), yi)
    across = at_chain(zi, fold - 1 - yi)

    def tp_peer(d):
        return tp + d - 2 * d * ((tp // d) % 2)

    def x_copy(d):
        if tps == 4:
            row = tp_peer(2) if d == 3 else tp
            peer = tp_peer(2) if d == 2 else tp_peer(1)
        else:
            row, peer = tp, lax.rem(tp + d, tps)
        return send(xall.at[row], xall.at[row], x_send.at[d], x_recv.at[d], {"tp": peer})

    def x_wait(d):
        if tps == 4:
            row = tps - 1 - tp if d == 3 else tp_peer(d)
        else:
            row = lax.rem(tp + tps - d, tps)
        peer = {"tp": lax.rem(tp + 1, tps)}
        send(xall.at[tp], xall.at[row], x_send.at[d], x_recv.at[d], peer).wait_recv()

    def w_up(k):
        src, dst = (reach - k) % reach, reach - k - 1
        return send(wo.at[src, 0], wo.at[dst, 0], wu_send.at[k], wz_recv.at[dst], above)

    def w_down(k):
        return send(wo.at[k, 0], wo.at[k + 1, 0], wd_send.at[k], wz_recv.at[k + 1], below)

    def w_across(r):
        return send(wo.at[r, 0], wo.at[r, 1], wy_send.at[r], wy_recv.at[r], across)

    def w_arrived(r):
        send(wo.at[r, 0], wo.at[r, 0], wy_send.at[r], wz_recv.at[r], above).wait_recv()

    def w_own():
        @pl.when(zi + 1 < reach)
        def _():
            w_up(0).start()

        @pl.when(zi >= 1)
        def _():
            w_down(0).start()

        if fold == 2:
            w_across(0).start()

    def w_relay(k):
        for there, r in ((zi >= k, reach - k), (zi + k < reach, k)):

            @pl.when(there)
            def _():
                w_arrived(r)

        if k + 1 < reach:

            @pl.when((zi >= k) & (zi + 1 < reach))
            def _():
                w_up(k).start()

            @pl.when((zi + k < reach) & (zi >= 1))
            def _():
                w_down(k).start()

        if fold == 2:
            for there, r in ((zi >= k, reach - k), (zi + k < reach, k)):

                @pl.when(there)
                def _():
                    w_across(r).start()

    def k_up(k):
        return send(kv.at[k, 0], kv.at[k + 1, 0], ku_send.at[k], kz_recv.at[k + 1], above)

    def k_across(k):
        return send(kv.at[k, 0], kv.at[k, 1], ky_send.at[k], ky_recv.at[k], across)

    def k_arrived(k):
        send(kv.at[k, 0], kv.at[k, 0], ky_send.at[k], kz_recv.at[k], above).wait_recv()

    def summary_copy(d):
        return send(
            summary.at[0],
            summary.at[d],
            s_send.at[d],
            s_recv.at[d],
            {"sp": lax.rem(li + d, chain) * seqs + seq},
        )

    def r_copy(slot, d, at):
        peer = lax.rem(tp + d, tps)
        return send(
            part.at[peer, :, pl.ds(at, cols)],
            landed.at[d, :, pl.ds(at, cols)],
            r_send.at[slot, d],
            r_recv.at[slot, d],
            {"tp": peer},
        )

    if tps == 4:
        x_copy(2).start()
        x_copy(1).start()
    else:
        for d in range(1, tps):
            x_copy(d).start()
    pulls[0].wait()
    pulls[1].wait()
    if gather:
        w_own()

    inner = iota((rows, 128), 1) % QK_DIM
    half = QK_DIM // 2
    power = (inner % half).astype(F32) * (-2.0 / QK_DIM)
    angle = (li * rows + iota((rows, 128), 0)).astype(F32) * jnp.exp(
        power * math.log(ROTARY_BASE)
    )
    cosine = jnp.cos(angle)
    sine = jnp.sin(angle)
    sine = jnp.where(inner < half, -sine, sine)

    def level(ref, first, count):
        return jnp.concatenate([ref[g : g + 1, :] for g in range(first, first + count)], axis=1)

    decay = level(decay_in, 0, groups)
    turn = level(turn_in, 0, groups)
    start_r, start_i = level(start_in, 0, groups), level(start_in, groups, groups)
    in_scale = jnp.sqrt(one_less_exp(2.0 * decay))
    straight = level(skip, 0, groups)

    keep = (iota((chans, flat), 0) // per) == (iota((chans, flat), 1) // states)

    def block_map(ref, which):
        tall = ref[which * chans : (which + 1) * chans, :]
        return jnp.where(keep, jnp.concatenate([tall] * groups, axis=1), 0.0)

    extra = extra_t[...].T
    lane = iota((rows, 2 * states), 1)
    pieces = [
        jnp.where(lane < states, extra[:, g : g + 1], extra[:, g + 1 : g + 2])
        for g in range(0, groups, 2)
    ]
    magnitude = jnp.exp(jnp.concatenate(pieces, axis=1) - decay)
    tr[...] = magnitude * jnp.cos(turn)
    ti[...] = magnitude * jnp.sin(turn)

    if tps == 4:
        x_wait(2)
        x_copy(3).start()
    for d in range(1, tps):
        if d != 2 or tps != 4:
            x_wait(d)
    for pull in pulls[2:]:
        pull.wait()
    x = xall[...].reshape(rows, width)

    def turned(raw):
        tiles = []
        first = inner < half
        for c in range(0, raw.shape[1], 128):
            v = raw[:, c : c + 128]
            other = jnp.where(first, pltpu.roll(v, 128 - half, 1), pltpu.roll(v, half, 1))
            tiles.append(v * cosine + other * sine)
        return tiles

    for i, tile in enumerate(turned(dot(x, wk[...]))):
        kv[0, 0, :, i * 128 : (i + 1) * 128] = tile.astype(BF16)
    kv[0, 0, :, qw:] = dot(x, wv[...]).astype(BF16)
    drive = dot(x, wd[...]).astype(BF16).astype(F32)

    @pl.when(zi + 1 < reach)
    def _():
        k_up(0).start()

    if fold == 2:

        @pl.when(yi == 0)
        def _():
            k_across(0).start()

    if gather and reach > 1:
        w_relay(1)

    for which, ref in enumerate((ir, ii)):
        ref[...] = in_scale * dot(drive, block_map(in_map, which), HIGHEST)

    def scan_tile(i, carry):
        mr, mi, ar, ai = carry
        at = pl.ds(pl.multiple_of(i * 8, 8), 8)
        a, b, u, v = tr[at, :], ti[at, :], ir[at, :], ii[at, :]
        rows_out = ([], [], [], [])
        for r in range(8):
            p, q = a[r : r + 1], b[r : r + 1]
            mr, mi = p * mr - q * mi, p * mi + q * mr
            ar, ai = (
                p * ar - q * ai + u[r : r + 1],
                p * ai + q * ar + v[r : r + 1],
            )
            for keep, value in zip(rows_out, (mr, mi, ar, ai)):
                keep.append(value)
        for ref, keep in zip((tr, ti, ir, ii), rows_out):
            ref[at, :] = jnp.concatenate(keep, axis=0)
        return mr, mi, ar, ai

    one, zero = jnp.ones((1, flat), F32), jnp.zeros((1, flat), F32)
    mr, mi, ar, ai = lax.fori_loop(0, rows // 8, scan_tile, (one, zero, zero, zero))
    head_of_chain = li == 0
    entry_r = mr * start_r - mi * start_i + ar
    entry_i = mr * start_i + mi * start_r + ai
    summary[0] = jnp.concatenate(
        (
            jnp.where(head_of_chain, 0.0, mr),
            jnp.where(head_of_chain, 0.0, mi),
            jnp.where(head_of_chain, entry_r, ar),
            jnp.where(head_of_chain, entry_i, ai),
            zero,
            zero,
            zero,
            zero,
        ),
        axis=0,
    )

    q_tiles = turned(dot(x, wq[...]))
    low = iota((rows, 128), 1) < QK_DIM
    for h in range(heads):
        tile = q_tiles[h].astype(BF16).astype(F32) * QK_DIM**-0.5
        qz[2 * h] = jnp.where(low, tile, 0.0).astype(BF16)
        qz[2 * h + 1] = jnp.where(low, 0.0, tile).astype(BF16)

    def push_summary(d, _):
        @pl.when(li + d < chain)
        def _():
            summary_copy(d).start()

        return 0

    lax.fori_loop(1, chain, push_summary, 0)

    def relay_kv(k):
        @pl.when(zi >= k)
        def _():
            k_arrived(k)
            if k + 1 < reach:

                @pl.when(zi + 1 < reach)
                def _():
                    k_up(k).start()

            if fold == 2:
                k_across(k).start()

    allowed = (iota((rows, rows), 1) // SEGMENT) <= (iota((rows, rows), 0) // SEGMENT)
    for u in range(2 * heads):
        h = u // 2
        s = dot_t(qz[u], kv[0, 0, :, h * 128 : (h + 1) * 128])
        s = jnp.where(allowed, s, MASK_FLOOR)
        m = jnp.max(s, axis=-1, keepdims=True)
        e = jnp.where(allowed, jnp.exp(s - m), 0.0)
        peak[u] = jnp.broadcast_to(m, (rows, V_DIM))
        total[u] = jnp.broadcast_to(jnp.sum(e, axis=-1, keepdims=True), (rows, V_DIM))
        numer[u] = dot(e.astype(BF16), kv[0, 0, :, qw + h * V_DIM : qw + (h + 1) * V_DIM])

    def attend(k, c):
        for u in range(2 * heads):
            h = u // 2
            s = dot_t(qz[u], kv[k, c, :, h * 128 : (h + 1) * 128])
            before = peak[u]
            m = jnp.maximum(before, jnp.max(s, axis=-1, keepdims=True))
            shrink = jnp.exp(before - m)
            e = jnp.exp(s - m[:, :1])
            peak[u] = m
            total[u] = total[u] * shrink + jnp.sum(e, axis=-1, keepdims=True)
            numer[u] = numer[u] * shrink + dot(
                e.astype(BF16), kv[k, c, :, qw + h * V_DIM : qw + (h + 1) * V_DIM]
            )

    def attend_across(k, there):
        @pl.when(there)
        def _():
            k_across(k).wait_recv()
            attend(k, 1)

    for k in range(1, reach):
        relay_kv(k)
        if gather and k >= 2:
            w_relay(k)
        if fold == 2:
            attend_across(k - 1, (zi >= k - 1) if k > 1 else (yi == 1))

        @pl.when(zi >= k)
        def _():
            attend(k, 0)

    if fold == 2:
        attend_across(reach - 1, (zi >= reach - 1) if reach > 1 else (yi == 1))

    for h in range(heads):
        diff = numer[2 * h] / total[2 * h] - mix[h] * (numer[2 * h + 1] / total[2 * h + 1])
        scale = lax.rsqrt(jnp.mean(diff * diff, axis=-1, keepdims=True) + EPSILON)
        acts[:, chans + h * V_DIM : chans + (h + 1) * V_DIM] = (
            diff * scale * sub_gain[...] * (1.0 - LAMBDA_INIT)
        ).astype(BF16)

    def enter(step, carry):
        j = chain - step

        def taken(carry):
            cr, ci = carry
            block = summary[j]
            a, b = block[0:1], block[1:2]
            return a * cr - b * ci + block[2:3], a * ci + b * cr + block[3:4]

        @pl.when(j <= li)
        def _():
            summary_copy(j).wait_recv()

        @pl.when(j > li)
        def _():
            summary[j] = jnp.zeros_like(summary[j])

        return taken(carry)

    cr, ci = lax.fori_loop(1, chain, enter, (zero, zero))
    cr = jnp.where(head_of_chain, start_r, cr)
    ci = jnp.where(head_of_chain, start_i, ci)
    state_r = tr[...] * cr - ti[...] * ci + ir[...]
    state_i = tr[...] * ci + ti[...] * cr + ii[...]
    blocks = [block_map(out_map, w) for w in range(2)]
    mixed = dot_t(state_r, blocks[0], HIGHEST) - dot_t(state_i, blocks[1], HIGHEST)
    acts[:, :chans] = jax.nn.gelu(mixed + straight * drive).astype(BF16)

    shares = [(r, c) for r in range(reach) for c in range(fold)] if gather else [(0, 0)]
    order = sorted(range(len(shares)), key=lambda i: min(shares[i][0], reach - shares[i][0]))

    def place(r, c):
        if not gather:
            return 0
        y = (yi + c) % fold
        return pl.multiple_of((lax.rem(zi + r, reach) * fold + y) * cols, 128)

    for i in order:
        r, c = shares[i]
        if c:
            w_across(r).wait_recv()
        block = dot(acts[...], wo[r, c])
        at = place(r, c)
        part[:, :, pl.ds(at, cols)] = block.astype(BF16).reshape(tps, own, cols)
        for d in range(1, tps):
            r_copy(i, d, at).start()
    summed = part[tp].astype(F32)
    for i in order:
        for d in range(1, tps):
            r_copy(i, d, place(*shares[i])).wait_recv()
    for d in range(1, tps):
        summed = summed + landed[d].astype(F32)
    out[...] = summed.astype(BF16)

    for d in range(1, tps):
        x_copy(d).wait_send()
        for i in order:
            r_copy(i, d, place(*shares[i])).wait_send()

    def drain(d, _):
        @pl.when(li + d < chain)
        def _():
            summary_copy(d).wait_send()

        return 0

    lax.fori_loop(1, chain, drain, 0)

    for k in range(reach):

        @pl.when((zi >= k) & (zi + 1 < reach))
        def _():
            if k + 1 < reach:
                k_up(k).wait_send()
                if gather:
                    w_up(k).wait_send()

        if gather:

            @pl.when((zi + k < reach) & (zi >= 1))
            def _():
                if k + 1 < reach:
                    w_down(k).wait_send()

        if fold == 2:

            @pl.when((zi >= k) if k else (yi == 0))
            def _():
                k_across(k).wait_send()

            if gather:
                w_across(k).wait_send()


def local(
    mesh_shape,
    tokens,
    norm_gain,
    w_query,
    w_key,
    w_value,
    w_state_in,
    decay_rate,
    rotation,
    extra_decay,
    in_map,
    out_map,
    skip_gain,
    init_state,
    mix_lambda,
    sub_gain,
    w_out_state,
    w_out_attn,
):
    sps, tps = mesh_shape
    seqs = init_state.shape[0]
    chain = sps // seqs
    own, width = tokens.shape
    rows = own * tps
    if rows % SEGMENT:
        raise ValueError("rows")
    groups, states = decay_rate.shape
    flat = groups * states
    chans = w_state_in.shape[1]
    qw = w_query.shape[1]
    vw = w_value.shape[1]
    units = 2 * vw // V_DIM
    sp = lax.axis_index("sp")
    fold = 2 if chain % 2 == 0 else 1
    reach = chain // fold
    gather = seqs == 1 and w_out_state.shape[1] % 128 == 0
    if not gather:
        w_out_state = lax.all_gather(w_out_state, "sp", axis=1, tiled=True)
        w_out_attn = lax.all_gather(w_out_attn, "sp", axis=1, tiled=True)
    cols = w_out_state.shape[1]
    shares = chain if gather else 1
    wo_shape = ((reach, fold) if gather else (1, 1)) + (chans + vw, cols)
    start = lax.dynamic_index_in_dim(init_state, sp % seqs, 0, keepdims=False)

    vmem = pl.BlockSpec(memory_space=pltpu.VMEM)
    hbm = pl.BlockSpec(memory_space=pl.ANY)
    smem = pl.BlockSpec(memory_space=pltpu.SMEM)
    dma = pltpu.SemaphoreType.DMA
    return pl.pallas_call(
        functools.partial(kernel, (seqs, chain, tps, fold, gather)),
        out_shape=jax.ShapeDtypeStruct((own, width), BF16),
        in_specs=[vmem, vmem, hbm, hbm, hbm, hbm]
        + [vmem] * 7
        + [smem, vmem, hbm, hbm],
        out_specs=vmem,
        scratch_shapes=[
            pltpu.VMEM((tps, own, width), BF16),
            pltpu.VMEM(w_query.shape, BF16),
            pltpu.VMEM(w_key.shape, BF16),
            pltpu.VMEM(w_value.shape, BF16),
            pltpu.VMEM(w_state_in.shape, BF16),
            pltpu.VMEM(wo_shape, BF16),
            pltpu.VMEM((units, rows, 128), BF16),
            pltpu.VMEM((reach, fold, rows, qw + vw), BF16),
            pltpu.VMEM((chain, 8, flat), F32),
            pltpu.VMEM((rows, flat), F32),
            pltpu.VMEM((rows, flat), F32),
            pltpu.VMEM((rows, flat), F32),
            pltpu.VMEM((rows, flat), F32),
            pltpu.VMEM((units, rows, V_DIM), F32),
            pltpu.VMEM((units, rows, V_DIM), F32),
            pltpu.VMEM((units, rows, V_DIM), F32),
            pltpu.VMEM((tps, own, width), BF16),
            pltpu.VMEM((tps, own, width), BF16),
            pltpu.VMEM((rows, chans + vw), BF16),
            dma((6,)),
            dma((tps,)),
            dma((tps,)),
            dma((reach,)),
            dma((reach,)),
            dma((reach,)),
            dma((reach,)),
            dma((reach,)),
            dma((reach,)),
            dma((reach,)),
            dma((reach,)),
            dma((reach,)),
            dma((chain,)),
            dma((chain,)),
            dma((shares, tps)),
            dma((shares, tps)),
        ],
        compiler_params=pltpu.CompilerParams(
            collective_id=0, has_side_effects=True, vmem_limit_bytes=67043328
        ),
    )(
        tokens,
        norm_gain.reshape(1, width),
        w_query,
        w_key,
        w_value,
        w_state_in,
        decay_rate,
        rotation,
        start.reshape(2 * groups, states),
        extra_decay.T,
        in_map.swapaxes(2, 3).reshape(2 * chans, states),
        out_map.reshape(2 * chans, states),
        skip_gain,
        mix_lambda,
        sub_gain.reshape(1, V_DIM),
        w_out_state,
        w_out_attn,
    )


def solution(mesh):
    in_specs = (
        P(("sp", "tp"), None),
        P(),
        P(None, "tp"),
        P(None, "tp"),
        P(None, "tp"),
        P(None, "tp"),
        P("tp", None),
        P("tp", None),
        P("sp", "tp"),
        P(None, "tp", None, None),
        P(None, "tp", None, None),
        P("tp", None),
        P(None, None, "tp", None),
        P("tp"),
        P(),
        P("tp", "sp"),
        P("tp", "sp"),
    )
    shape = (mesh.shape["sp"], mesh.shape["tp"])
    return jax.shard_map(
        functools.partial(local, shape),
        mesh=mesh,
        in_specs=in_specs,
        out_specs=P(("sp", "tp"), None),
        check_vma=False,
    )
```

```python
import functools
import math

import jax
import jax.numpy as jnp
from jax import lax
from jax.experimental import pallas as pl
from jax.experimental.pallas import tpu as pltpu
from jax.sharding import PartitionSpec as P

QK_DIM = 64
V_DIM = 128
SEGMENT = 64
EPSILON = 1e-06
ROTARY_BASE = 10000.0
LAMBDA_INIT = 0.2
MASK_FLOOR = -1e30
F32 = jnp.float32
BF16 = jnp.bfloat16
MESH = pl.DeviceIdType.MESH
HIGHEST = lax.Precision.HIGHEST


def dot(a, b, precision=None):
    return jnp.dot(a, b, preferred_element_type=F32, precision=precision)


def dot_t(a, b, precision=None):
    return lax.dot_general(
        a, b, (((1,), (1,)), ((), ())), preferred_element_type=F32, precision=precision
    )


def one_less_exp(x):
    series = jnp.ones_like(x)
    for n in range(9, 1, -1):
        series = 1.0 - x * series * (1.0 / n)
    return jnp.where(x < 0.5, x * series, 1.0 - jnp.exp(-x))


def iota(shape, axis):
    return lax.broadcasted_iota(jnp.int32, shape, axis)


def kernel(
    cfg,
    tokens,
    gain,
    wq_hbm,
    wk_hbm,
    wv_hbm,
    wd_hbm,
    decay_in,
    turn_in,
    start_in,
    extra_t,
    in_map,
    out_map,
    skip,
    mix,
    sub_gain,
    ws_hbm,
    wa_hbm,
    out,
    xall,
    wq,
    wk,
    wv,
    wd,
    wo,
    qz,
    kv,
    summary,
    tr,
    ti,
    ir,
    ii,
    peak,
    total,
    numer,
    part,
    landed,
    acts,
    local_sem,
    x_send,
    x_recv,
    wu_send,
    wd_send,
    wy_send,
    wz_recv,
    wy_recv,
    ku_send,
    ky_send,
    kz_recv,
    ky_recv,
    s_send,
    s_recv,
    r_send,
    r_recv,
):
    seqs, chain, tps, fold, gather = cfg
    reach = chain // fold
    sp = lax.axis_index("sp")
    tp = lax.axis_index("tp")
    li = sp // seqs
    seq = sp % seqs
    zi, yi = li // fold, li % fold
    own, width = tokens.shape
    rows = own * tps
    heads = wv.shape[1] // V_DIM
    qw = wq.shape[1]
    cols = wo.shape[3]
    flat = tr.shape[1]
    groups = extra_t.shape[0]
    states = flat // groups
    chans = wd.shape[1]
    per = chans // groups

    pulls = [
        pltpu.make_async_copy(src, dst, local_sem.at[i])
        for i, (src, dst) in enumerate(
            (
                (ws_hbm, wo.at[0, 0, pl.ds(0, chans)]),
                (wa_hbm, wo.at[0, 0, pl.ds(chans, wa_hbm.shape[0])]),
                (wd_hbm, wd),
                (wk_hbm, wk),
                (wv_hbm, wv),
                (wq_hbm, wq),
            )
        )
    ]
    for pull in pulls:
        pull.start()

    barrier = pltpu.get_barrier_semaphore()

    def greet_tp(d, _):
        pl.semaphore_signal(
            barrier, inc=1, device_id={"tp": lax.rem(tp + d, tps)}, device_id_type=MESH
        )
        return 0

    def greet_sp(d, _):
        pl.semaphore_signal(
            barrier,
            inc=1,
            device_id={"sp": lax.rem(li + d, chain) * seqs + seq},
            device_id_type=MESH,
        )
        return 0

    lax.fori_loop(1, tps, greet_tp, 0)
    lax.fori_loop(1, chain, greet_sp, 0)

    wide = tokens[...].astype(F32)
    scale = lax.rsqrt(jnp.mean(wide * wide, axis=-1, keepdims=True) + EPSILON)
    xall[tp] = (wide * scale * gain[...]).astype(BF16)

    pl.semaphore_wait(barrier, tps - 1 + chain - 1)

    def send(src, dst, send_sem, recv_sem, device_id):
        return pltpu.make_async_remote_copy(
            src_ref=src,
            dst_ref=dst,
            send_sem=send_sem,
            recv_sem=recv_sem,
            device_id=device_id,
            device_id_type=MESH,
        )

    def at_chain(z, y):
        return {"sp": (z * fold + y) * seqs + seq}

    above = at_chain(lax.rem(zi + 1, reach), yi)
    below = at_chain(lax.rem(zi + reach - 1, reach), yi)
    across = at_chain(zi, fold - 1 - yi)

    def tp_peer(d):
        return tp + d - 2 * d * ((tp // d) % 2)

    def x_copy(d):
        if tps == 4:
            row = tp_peer(2) if d == 3 else tp
            peer = tp_peer(2) if d == 2 else tp_peer(1)
        else:
            row, peer = tp, lax.rem(tp + d, tps)
        return send(xall.at[row], xall.at[row], x_send.at[d], x_recv.at[d], {"tp": peer})

    def x_wait(d):
        if tps == 4:
            row = tps - 1 - tp if d == 3 else tp_peer(d)
        else:
            row = lax.rem(tp + tps - d, tps)
        peer = {"tp": lax.rem(tp + 1, tps)}
        send(xall.at[tp], xall.at[row], x_send.at[d], x_recv.at[d], peer).wait_recv()

    def w_up(k):
        src, dst = (reach - k) % reach, reach - k - 1
        return send(wo.at[src, 0], wo.at[dst, 0], wu_send.at[k], wz_recv.at[dst], above)

    def w_down(k):
        return send(wo.at[k, 0], wo.at[k + 1, 0], wd_send.at[k], wz_recv.at[k + 1], below)

    def w_across(r):
        return send(wo.at[r, 0], wo.at[r, 1], wy_send.at[r], wy_recv.at[r], across)

    def w_arrived(r):
        send(wo.at[r, 0], wo.at[r, 0], wy_send.at[r], wz_recv.at[r], above).wait_recv()

    def w_own():
        @pl.when(zi + 1 < reach)
        def _():
            w_up(0).start()

        @pl.when(zi >= 1)
        def _():
            w_down(0).start()

        if fold == 2:
            w_across(0).start()

    def w_relay(k):
        for there, r in ((zi >= k, reach - k), (zi + k < reach, k)):

            @pl.when(there)
            def _():
                w_arrived(r)

        if k + 1 < reach:

            @pl.when((zi >= k) & (zi + 1 < reach))
            def _():
                w_up(k).start()

            @pl.when((zi + k < reach) & (zi >= 1))
            def _():
                w_down(k).start()

        if fold == 2:
            for there, r in ((zi >= k, reach - k), (zi + k < reach, k)):

                @pl.when(there)
                def _():
                    w_across(r).start()

    def k_up(k):
        return send(kv.at[k, 0], kv.at[k + 1, 0], ku_send.at[k], kz_recv.at[k + 1], above)

    def k_across(k):
        return send(kv.at[k, 0], kv.at[k, 1], ky_send.at[k], ky_recv.at[k], across)

    def k_arrived(k):
        send(kv.at[k, 0], kv.at[k, 0], ky_send.at[k], kz_recv.at[k], above).wait_recv()

    def summary_copy(d):
        return send(
            summary.at[0],
            summary.at[d],
            s_send.at[d],
            s_recv.at[d],
            {"sp": lax.rem(li + d, chain) * seqs + seq},
        )

    def r_copy(slot, d, at):
        peer = lax.rem(tp + d, tps)
        return send(
            part.at[peer, :, pl.ds(at, cols)],
            landed.at[d, :, pl.ds(at, cols)],
            r_send.at[slot, d],
            r_recv.at[slot, d],
            {"tp": peer},
        )

    if tps == 4:
        x_copy(2).start()
        x_copy(1).start()
    else:
        for d in range(1, tps):
            x_copy(d).start()
    pulls[0].wait()
    pulls[1].wait()
    if gather:
        w_own()

    inner = iota((rows, 128), 1) % QK_DIM
    half = QK_DIM // 2
    power = (inner % half).astype(F32) * (-2.0 / QK_DIM)
    angle = (li * rows + iota((rows, 128), 0)).astype(F32) * jnp.exp(
        power * math.log(ROTARY_BASE)
    )
    cosine = jnp.cos(angle)
    sine = jnp.sin(angle)
    sine = jnp.where(inner < half, -sine, sine)

    def level(ref, first, count):
        return jnp.concatenate([ref[g : g + 1, :] for g in range(first, first + count)], axis=1)

    decay = level(decay_in, 0, groups)
    turn = level(turn_in, 0, groups)
    start_r, start_i = level(start_in, 0, groups), level(start_in, groups, groups)
    in_scale = jnp.sqrt(one_less_exp(2.0 * decay))
    straight = level(skip, 0, groups)

    keep = (iota((chans, flat), 0) // per) == (iota((chans, flat), 1) // states)

    def block_map(ref, which):
        tall = ref[which * chans : (which + 1) * chans, :]
        return jnp.where(keep, jnp.concatenate([tall] * groups, axis=1), 0.0)

    extra = extra_t[...].T
    lane = iota((rows, 2 * states), 1)
    pieces = [
        jnp.where(lane < states, extra[:, g : g + 1], extra[:, g + 1 : g + 2])
        for g in range(0, groups, 2)
    ]
    magnitude = jnp.exp(jnp.concatenate(pieces, axis=1) - decay)
    tr[...] = magnitude * jnp.cos(turn)
    ti[...] = magnitude * jnp.sin(turn)

    if tps == 4:
        x_wait(2)
        x_copy(3).start()
    for d in range(1, tps):
        if d != 2 or tps != 4:
            x_wait(d)
    for pull in pulls[2:]:
        pull.wait()
    x = xall[...].reshape(rows, width)

    def turned(raw):
        tiles = []
        first = inner < half
        for c in range(0, raw.shape[1], 128):
            v = raw[:, c : c + 128]
            other = jnp.where(first, pltpu.roll(v, 128 - half, 1), pltpu.roll(v, half, 1))
            tiles.append(v * cosine + other * sine)
        return tiles

    for i, tile in enumerate(turned(dot(x, wk[...]))):
        kv[0, 0, :, i * 128 : (i + 1) * 128] = tile.astype(BF16)
    if gather and reach > 1:
        w_relay(1)
    kv[0, 0, :, qw:] = dot(x, wv[...]).astype(BF16)
    drive = dot(x, wd[...]).astype(BF16).astype(F32)

    @pl.when(zi + 1 < reach)
    def _():
        k_up(0).start()

    if fold == 2:

        @pl.when(yi == 0)
        def _():
            k_across(0).start()

    for which, ref in enumerate((ir, ii)):
        ref[...] = in_scale * dot(drive, block_map(in_map, which), HIGHEST)

    def scan_tile(i, carry):
        mr, mi, ar, ai = carry
        at = pl.ds(pl.multiple_of(i * 8, 8), 8)
        a, b, u, v = tr[at, :], ti[at, :], ir[at, :], ii[at, :]
        rows_out = ([], [], [], [])
        for r in range(8):
            p, q = a[r : r + 1], b[r : r + 1]
            mr, mi = p * mr - q * mi, p * mi + q * mr
            ar, ai = (
                p * ar - q * ai + u[r : r + 1],
                p * ai + q * ar + v[r : r + 1],
            )
            for keep, value in zip(rows_out, (mr, mi, ar, ai)):
                keep.append(value)
        for ref, keep in zip((tr, ti, ir, ii), rows_out):
            ref[at, :] = jnp.concatenate(keep, axis=0)
        return mr, mi, ar, ai

    one, zero = jnp.ones((1, flat), F32), jnp.zeros((1, flat), F32)
    mr, mi, ar, ai = lax.fori_loop(0, rows // 8, scan_tile, (one, zero, zero, zero))
    head_of_chain = li == 0
    entry_r = mr * start_r - mi * start_i + ar
    entry_i = mr * start_i + mi * start_r + ai
    summary[0] = jnp.concatenate(
        (
            jnp.where(head_of_chain, 0.0, mr),
            jnp.where(head_of_chain, 0.0, mi),
            jnp.where(head_of_chain, entry_r, ar),
            jnp.where(head_of_chain, entry_i, ai),
            zero,
            zero,
            zero,
            zero,
        ),
        axis=0,
    )

    q_tiles = turned(dot(x, wq[...]))
    low = iota((rows, 128), 1) < QK_DIM
    for h in range(heads):
        tile = q_tiles[h].astype(BF16).astype(F32) * QK_DIM**-0.5
        qz[2 * h] = jnp.where(low, tile, 0.0).astype(BF16)
        qz[2 * h + 1] = jnp.where(low, 0.0, tile).astype(BF16)

    def push_summary(d, _):
        @pl.when(li + d < chain)
        def _():
            summary_copy(d).start()

        return 0

    lax.fori_loop(1, chain, push_summary, 0)

    def relay_kv(k):
        @pl.when(zi >= k)
        def _():
            k_arrived(k)
            if k + 1 < reach:

                @pl.when(zi + 1 < reach)
                def _():
                    k_up(k).start()

            if fold == 2:
                k_across(k).start()

    allowed = (iota((rows, rows), 1) // SEGMENT) <= (iota((rows, rows), 0) // SEGMENT)
    for u in range(2 * heads):
        h = u // 2
        s = dot_t(qz[u], kv[0, 0, :, h * 128 : (h + 1) * 128])
        s = jnp.where(allowed, s, MASK_FLOOR)
        m = jnp.max(s, axis=-1, keepdims=True)
        e = jnp.where(allowed, jnp.exp(s - m), 0.0)
        peak[u] = jnp.broadcast_to(m, (rows, V_DIM))
        total[u] = jnp.broadcast_to(jnp.sum(e, axis=-1, keepdims=True), (rows, V_DIM))
        numer[u] = dot(e.astype(BF16), kv[0, 0, :, qw + h * V_DIM : qw + (h + 1) * V_DIM])

    def attend(k, c):
        for u in range(2 * heads):
            h = u // 2
            s = dot_t(qz[u], kv[k, c, :, h * 128 : (h + 1) * 128])
            before = peak[u]
            m = jnp.maximum(before, jnp.max(s, axis=-1, keepdims=True))
            shrink = jnp.exp(before - m)
            e = jnp.exp(s - m[:, :1])
            peak[u] = m
            total[u] = total[u] * shrink + jnp.sum(e, axis=-1, keepdims=True)
            numer[u] = numer[u] * shrink + dot(
                e.astype(BF16), kv[k, c, :, qw + h * V_DIM : qw + (h + 1) * V_DIM]
            )

    def attend_across(k, there):
        @pl.when(there)
        def _():
            k_across(k).wait_recv()
            attend(k, 1)

    def state_branch():
        def enter(step, carry):
            j = chain - step

            def taken(carry):
                cr, ci = carry
                block = summary[j]
                a, b = block[0:1], block[1:2]
                return a * cr - b * ci + block[2:3], a * ci + b * cr + block[3:4]

            @pl.when(j <= li)
            def _():
                summary_copy(j).wait_recv()

            @pl.when(j > li)
            def _():
                summary[j] = jnp.zeros_like(summary[j])

            return taken(carry)

        cr, ci = lax.fori_loop(1, chain, enter, (zero, zero))
        cr = jnp.where(head_of_chain, start_r, cr)
        ci = jnp.where(head_of_chain, start_i, ci)
        state_r = tr[...] * cr - ti[...] * ci + ir[...]
        state_i = tr[...] * ci + ti[...] * cr + ii[...]
        blocks = [block_map(out_map, w) for w in range(2)]
        mixed = dot_t(state_r, blocks[0], HIGHEST) - dot_t(state_i, blocks[1], HIGHEST)
        acts[:, :chans] = jax.nn.gelu(mixed + straight * drive).astype(BF16)

    if reach == 1:
        state_branch()
    for k in range(1, reach):
        relay_kv(k)
        if gather and k + 1 < reach - 1:
            w_relay(k + 1)
        if gather and k == reach - 1 and k > 1:
            w_relay(k)
        if k == reach - 1:
            state_branch()
        if fold == 2:
            attend_across(k - 1, (zi >= k - 1) if k > 1 else (yi == 1))

        @pl.when(zi >= k)
        def _():
            attend(k, 0)

    if fold == 2:
        attend_across(reach - 1, (zi >= reach - 1) if reach > 1 else (yi == 1))

    for h in range(heads):
        diff = numer[2 * h] / total[2 * h] - mix[h] * (numer[2 * h + 1] / total[2 * h + 1])
        scale = lax.rsqrt(jnp.mean(diff * diff, axis=-1, keepdims=True) + EPSILON)
        acts[:, chans + h * V_DIM : chans + (h + 1) * V_DIM] = (
            diff * scale * sub_gain[...] * (1.0 - LAMBDA_INIT)
        ).astype(BF16)

    shares = [(r, c) for r in range(reach) for c in range(fold)] if gather else [(0, 0)]
    shares.sort(key=lambda share: (share[0] > 0, share[1], share[0]))
    order = range(len(shares))

    def nearest_first(r):
        return jnp.where(2 * zi >= reach, (reach - r) % reach, r) if r else 0

    def place(r, c):
        if not gather:
            return 0
        y = (yi + c) % fold
        return pl.multiple_of((lax.rem(zi + r, reach) * fold + y) * cols, 128)

    for i in order:
        r, c = nearest_first(shares[i][0]), shares[i][1]
        if c:
            w_across(r).wait_recv()
        block = dot(acts[...], wo[r, c])
        at = place(r, c)
        part[:, :, pl.ds(at, cols)] = block.astype(BF16).reshape(tps, own, cols)
        for d in range(1, tps):
            r_copy(i, d, at).start()
    summed = part[tp].astype(F32)
    for i in order:
        for d in range(1, tps):
            r_copy(i, d, place(nearest_first(shares[i][0]), shares[i][1])).wait_recv()
    for d in range(1, tps):
        summed = summed + landed[d].astype(F32)
    out[...] = summed.astype(BF16)

    for d in range(1, tps):
        x_copy(d).wait_send()
        for i in order:
            r_copy(i, d, place(nearest_first(shares[i][0]), shares[i][1])).wait_send()

    def drain(d, _):
        @pl.when(li + d < chain)
        def _():
            summary_copy(d).wait_send()

        return 0

    lax.fori_loop(1, chain, drain, 0)

    for k in range(reach):

        @pl.when((zi >= k) & (zi + 1 < reach))
        def _():
            if k + 1 < reach:
                k_up(k).wait_send()
                if gather:
                    w_up(k).wait_send()

        if gather:

            @pl.when((zi + k < reach) & (zi >= 1))
            def _():
                if k + 1 < reach:
                    w_down(k).wait_send()

        if fold == 2:

            @pl.when((zi >= k) if k else (yi == 0))
            def _():
                k_across(k).wait_send()

            if gather:
                w_across(k).wait_send()


def local(
    mesh_shape,
    tokens,
    norm_gain,
    w_query,
    w_key,
    w_value,
    w_state_in,
    decay_rate,
    rotation,
    extra_decay,
    in_map,
    out_map,
    skip_gain,
    init_state,
    mix_lambda,
    sub_gain,
    w_out_state,
    w_out_attn,
):
    sps, tps = mesh_shape
    seqs = init_state.shape[0]
    chain = sps // seqs
    own, width = tokens.shape
    rows = own * tps
    if rows % SEGMENT:
        raise ValueError("rows")
    groups, states = decay_rate.shape
    flat = groups * states
    chans = w_state_in.shape[1]
    qw = w_query.shape[1]
    vw = w_value.shape[1]
    units = 2 * vw // V_DIM
    sp = lax.axis_index("sp")
    fold = 2 if chain % 2 == 0 else 1
    reach = chain // fold
    gather = seqs == 1 and w_out_state.shape[1] % 128 == 0
    if not gather:
        w_out_state = lax.all_gather(w_out_state, "sp", axis=1, tiled=True)
        w_out_attn = lax.all_gather(w_out_attn, "sp", axis=1, tiled=True)
    cols = w_out_state.shape[1]
    shares = chain if gather else 1
    wo_shape = ((reach, fold) if gather else (1, 1)) + (chans + vw, cols)
    start = lax.dynamic_index_in_dim(init_state, sp % seqs, 0, keepdims=False)

    vmem = pl.BlockSpec(memory_space=pltpu.VMEM)
    hbm = pl.BlockSpec(memory_space=pl.ANY)
    smem = pl.BlockSpec(memory_space=pltpu.SMEM)
    dma = pltpu.SemaphoreType.DMA
    return pl.pallas_call(
        functools.partial(kernel, (seqs, chain, tps, fold, gather)),
        out_shape=jax.ShapeDtypeStruct((own, width), BF16),
        in_specs=[vmem, vmem, hbm, hbm, hbm, hbm]
        + [vmem] * 7
        + [smem, vmem, hbm, hbm],
        out_specs=vmem,
        scratch_shapes=[
            pltpu.VMEM((tps, own, width), BF16),
            pltpu.VMEM(w_query.shape, BF16),
            pltpu.VMEM(w_key.shape, BF16),
            pltpu.VMEM(w_value.shape, BF16),
            pltpu.VMEM(w_state_in.shape, BF16),
            pltpu.VMEM(wo_shape, BF16),
            pltpu.VMEM((units, rows, 128), BF16),
            pltpu.VMEM((reach, fold, rows, qw + vw), BF16),
            pltpu.VMEM((chain, 8, flat), F32),
            pltpu.VMEM((rows, flat), F32),
            pltpu.VMEM((rows, flat), F32),
            pltpu.VMEM((rows, flat), F32),
            pltpu.VMEM((rows, flat), F32),
            pltpu.VMEM((units, rows, V_DIM), F32),
            pltpu.VMEM((units, rows, V_DIM), F32),
            pltpu.VMEM((units, rows, V_DIM), F32),
            pltpu.VMEM((tps, own, width), BF16),
            pltpu.VMEM((tps, own, width), BF16),
            pltpu.VMEM((rows, chans + vw), BF16),
            dma((6,)),
            dma((tps,)),
            dma((tps,)),
            dma((reach,)),
            dma((reach,)),
            dma((reach,)),
            dma((reach,)),
            dma((reach,)),
            dma((reach,)),
            dma((reach,)),
            dma((reach,)),
            dma((reach,)),
            dma((chain,)),
            dma((chain,)),
            dma((shares, tps)),
            dma((shares, tps)),
        ],
        compiler_params=pltpu.CompilerParams(
            collective_id=0, has_side_effects=True, vmem_limit_bytes=67043328
        ),
    )(
        tokens,
        norm_gain.reshape(1, width),
        w_query,
        w_key,
        w_value,
        w_state_in,
        decay_rate,
        rotation,
        start.reshape(2 * groups, states),
        extra_decay.T,
        in_map.swapaxes(2, 3).reshape(2 * chans, states),
        out_map.reshape(2 * chans, states),
        skip_gain,
        mix_lambda,
        sub_gain.reshape(1, V_DIM),
        w_out_state,
        w_out_attn,
    )


def solution(mesh):
    in_specs = (
        P(("sp", "tp"), None),
        P(),
        P(None, "tp"),
        P(None, "tp"),
        P(None, "tp"),
        P(None, "tp"),
        P("tp", None),
        P("tp", None),
        P("sp", "tp"),
        P(None, "tp", None, None),
        P(None, "tp", None, None),
        P("tp", None),
        P(None, None, "tp", None),
        P("tp"),
        P(),
        P("tp", "sp"),
        P("tp", "sp"),
    )
    shape = (mesh.shape["sp"], mesh.shape["tp"])
    return jax.shard_map(
        functools.partial(local, shape),
        mesh=mesh,
        in_specs=in_specs,
        out_specs=P(("sp", "tp"), None),
        check_vma=False,
    )
```
